128 devices in a mesh: tp: 16 (over z, x), dp: 8 (over y, core).
Axes of the slice: x: 4, y: 4, z: 4, core: 2. Of those that a mesh axis runs over, the one named last changes fastest.
Arguments:
- stream_in: bfloat16 [256, 4096], P('tp', 'dp'), may hold values from -21 to 21
- hidden_state: float32 [2, 256, 4096], P(None, 'dp', 'tp'), may hold values from -6 to 6
- convolution_window_state: bfloat16 [2, 256, 3, 4096], P(None, 'dp', None, 'tp'), may hold values from -6 to 6
- norm_gain: float32 [2, 4096], P(None, 'dp'), may hold values from 0.1 to 1.9
- path_weight: bfloat16 [2, 4096, 4096], P(None, 'dp', 'tp'), may hold values from -0.09375 to 0.09375
- output_gate_weight: bfloat16 [2, 4096, 4096], P(None, 'dp', 'tp'), may hold values from -0.09375 to 0.09375
- conv_taps: float32 [2, 4, 4096], P(None, None, 'tp'), may hold values from -3 to 3
- recur_map: float32 [2, 64, 64, 64], P(None, 'tp'), may hold values from -0.75 to 0.75
- input_map: float32 [2, 64, 64, 64], P(None, 'tp'), may hold values from -0.75 to 0.75
- decay_logit: float32 [2, 4096], P(None, 'tp'), may hold values from 1 to 6
- out_weight: bfloat16 [2, 4096, 4096], P(None, 'tp', 'dp'), may hold values from -0.09375 to 0.09375
Outputs:
- stream_out: bfloat16 [256, 4096], P('tp', 'dp')
- hidden_next: float32 [2, 256, 4096], P(None, 'dp', 'tp')
- conv_next: bfloat16 [2, 256, 3, 4096], P(None, 'dp', None, 'tp')
The draws below stay inside these ranges and needn't reach their ends.
All inputs are finite; a program needn't handle non-finite values.
Results may differ from the reference program's by a relative error of at most 0.019.
Values may be sent and summed in bfloat16 or wider, within the bound.
No kernel may reach another device: no remote copies, remote signals or barrier semaphores. Data moves between devices by JAX's collectives and lax.ppermute only.
A program may use at most 64 MiB of HBM per device.

```python
import jax
import jax.numpy as jnp
from jax import lax

D = 4096
R = 4096
BLOCK_W = 64
NBLK = 64
LAYERS = 2
TAPS = 4
BATCH = 256
N_DP = 8


def draw_stream_in(key, part):
    first, second = jax.random.split(key, 2)
    groups = D // 64
    group_scale = jnp.exp(jax.random.uniform(first, (groups,), jnp.float32, jnp.log(0.3), jnp.log(3.0)))
    column_scale = jnp.repeat(group_scale, 64)
    values = jnp.clip(jax.random.normal(second, (BATCH, D), jnp.float32), -4.0, 4.0)
    return (values * column_scale[None, :]).astype(jnp.bfloat16)


def level_of(rng, dims, cuts, low, largest):
    loudness = 1.0
    for axis_at, shards_of in cuts:
        steps = jax.random.uniform(jax.random.fold_in(jax.random.fold_in(rng, 6), axis_at), (shards_of,), jnp.float32, low / len(cuts), largest / len(cuts))
        loudness = loudness * jnp.repeat(jnp.exp(steps), dims[axis_at] // shards_of).reshape((-1,) + (1,) * (len(dims) - 1 - axis_at))
    return loudness


def scatter_about(rng, extent, scale, most, shards=(), dtype=jnp.bfloat16):
    factor_of = level_of(rng, extent, shards, -0.22, 0.18) if shards else 1.0
    drawn = jax.random.normal(rng, extent, jnp.float32) * scale * factor_of
    return jnp.minimum(jnp.maximum(drawn, -most), most).astype(dtype)


def setup_inputs(seed: int = 0) -> dict:
    streams_of = jax.random.split(jax.random.key(seed), 12)
    return {
        "stream_in": draw_stream_in(jax.random.fold_in(streams_of[11], 71), 0),
        "hidden_state": scatter_about(streams_of[1], (LAYERS, BATCH, R), 1.0, 6.0, ((1, 8), (2, 16)), jnp.float32),
        "convolution_window_state": scatter_about(streams_of[2], (LAYERS, BATCH, TAPS - 1, R), 1.0, 6.0, ((1, 8), (3, 16))),
        "norm_gain": jnp.clip(1.0 + 0.18 * jax.random.normal(streams_of[3], (LAYERS, D), jnp.float32), 0.1, 1.9),
        "path_weight": scatter_about(streams_of[4], (LAYERS, D, R), D ** -0.5, 0.09375, ((1, 8), (2, 16))),
        "output_gate_weight": scatter_about(streams_of[5], (LAYERS, D, R), D ** -0.5, 0.09375, ((1, 8), (2, 16))),
        "conv_taps": scatter_about(streams_of[6], (LAYERS, TAPS, R), 0.5, 3.0, ((2, 16),), jnp.float32),
        "recur_map": scatter_about(streams_of[7], (LAYERS, NBLK, BLOCK_W, BLOCK_W), BLOCK_W ** -0.5, 0.75, ((1, 16),), jnp.float32),
        "input_map": scatter_about(streams_of[8], (LAYERS, NBLK, BLOCK_W, BLOCK_W), BLOCK_W ** -0.5, 0.75, ((1, 16),), jnp.float32),
        "decay_logit": jnp.clip(1.0 + 5.0 * jax.random.uniform(streams_of[9], (LAYERS, R), jnp.float32) ** level_of(streams_of[9], (LAYERS, R), ((1, 16),), -0.2, 0.2), 1.0, 6.0),
        "out_weight": scatter_about(streams_of[10], (LAYERS, R, D), R ** -0.5, 0.09375, ((1, 16), (2, 8))),
    }


EPS = 1e-06

def one_block(stream, hidden, buffer, gain, path_w, gate_branch_matrix, taps, recur_w, input_matrix, logit, out_w):
    batch = stream.shape[0]
    streamf = stream.astype(jnp.float32)
    sumsq = lax.optimization_barrier(jnp.sum(streamf * streamf, axis=1))
    normed = (streamf * lax.rsqrt(sumsq / D + EPS)[:, None] * gain[None, :]).astype(jnp.bfloat16)
    block_list = normed.astype(jnp.float32).reshape(batch, N_DP, D // N_DP)

    def summed(weight):
        weight_block_list = weight.astype(jnp.float32).reshape(N_DP, D // N_DP, R)
        piece_list = jnp.einsum('yiq,iqx->iyx', block_list, weight_block_list).astype(jnp.bfloat16)
        piece_list = lax.optimization_barrier(piece_list).astype(jnp.float32)
        return lax.optimization_barrier(jnp.sum(piece_list, axis=0)).astype(jnp.bfloat16)
    zpath = summed(path_w)
    zgate = summed(gate_branch_matrix)
    conv = zpath.astype(jnp.float32) * taps[TAPS - 1][None, :]
    for j in range(TAPS - 1):
        conv = conv + buffer[:, j].astype(jnp.float32) * taps[j][None, :]
    new_buffer = jnp.concatenate([buffer[:, 1:], zpath[:, None, :]], axis=1)
    cblocks = conv.reshape(batch, NBLK, BLOCK_W)
    rgate = jax.nn.sigmoid(jnp.einsum('bnc,ncd->bnd', cblocks, recur_w, precision=lax.Precision.HIGHEST).reshape(batch, R))
    igate = jax.nn.sigmoid(jnp.einsum('bnc,ncd->bnd', cblocks, input_matrix, precision=lax.Precision.HIGHEST).reshape(batch, R))
    loga = 8.0 * rgate * jax.nn.log_sigmoid(logit)[None, :]
    new_hidden = jnp.exp(loga) * hidden + jnp.sqrt(-jnp.expm1(2.0 * loga)) * (igate * conv)
    mixed = (new_hidden * jax.nn.gelu(zgate.astype(jnp.float32))).astype(jnp.bfloat16)
    update = jnp.dot(mixed, out_w, preferred_element_type=jnp.float32)
    return ((streamf + update).astype(jnp.bfloat16), new_hidden, new_buffer)

def reference(stream_in, hidden_state, convolution_window_state, norm_gain, path_weight, output_gate_weight, conv_taps, recur_map, input_map, decay_logit, out_weight):
    stream = stream_in
    hiddens = []
    buffers = []
    for layer in range(LAYERS):
        stream, new_hidden, new_buffer = one_block(stream, hidden_state[layer], convolution_window_state[layer], norm_gain[layer], path_weight[layer], output_gate_weight[layer], conv_taps[layer], recur_map[layer], input_map[layer], decay_logit[layer], out_weight[layer])
        hiddens.append(new_hidden)
        buffers.append(new_buffer)
    return (stream, jnp.stack(hiddens), jnp.stack(buffers))
```

```python
import jax
import jax.numpy as jnp
from jax import lax
from jax.sharding import PartitionSpec as P

D = 4096
TAPS = 4


EPS = 1e-06


def from_everyone(array, axis):
    copies = jnp.broadcast_to(array, (lax.axis_size(axis), *array.shape))
    return lax.all_to_all(copies, axis, split_axis=0, concat_axis=0, tiled=True)


def of_everyone(array, axis):
    everything = from_everyone(array, axis)
    return jnp.sum(everything, axis=0)


def in_order(parts, dim):
    parts = jnp.moveaxis(parts, 0, dim)
    shape = parts.shape
    return parts.reshape(*shape[:dim], shape[dim] * shape[dim + 1], *shape[dim + 2 :])


def collect(array, axis, dim):
    return in_order(from_everyone(array, axis), dim)


def in_blocks(array, dim, devices):
    before, after = (array.shape[:dim], array.shape[dim + 1 :])
    return jnp.moveaxis(array.reshape(*before, devices, -1, *after), dim, 0)


def sum_at_owner(array, axis, dim):
    parts = in_blocks(array, dim, lax.axis_size(axis))
    arrived = lax.all_to_all(parts, axis, split_axis=0, concat_axis=0, tiled=True)
    return arrived.astype(jnp.float32).sum(axis=0)


def split_inputs(rows, gain, path_w, gate_branch_matrix):
    everyone = collect(rows, "tp", 0).astype(jnp.float32)
    sumsq = jnp.sum(everyone * everyone, axis=1, keepdims=True)
    high = lax.reduce_precision(sumsq, 8, 7)
    low = sumsq - high
    gained = (everyone * gain[None, :]).astype(jnp.bfloat16)
    return jnp.concatenate(
        [
            jnp.dot(gained, path_w, preferred_element_type=jnp.float32),
            jnp.dot(gained, gate_branch_matrix, preferred_element_type=jnp.float32),
            high,
            low,
            jnp.zeros((sumsq.shape[0], 126), jnp.float32),
        ],
        axis=1,
    )


def recur_tail(partial_value, hidden, buffer, taps, recur_w, input_matrix, logit, out_w):
    width = (partial_value.shape[1] - 128) // 2
    summed = sum_at_owner(partial_value.astype(jnp.bfloat16), "dp", 0)
    sumsq = summed[:, 2 * width] + summed[:, 2 * width + 1]
    factor = lax.rsqrt(sumsq / D + EPS)[:, None]
    zpath = (summed[:, :width] * factor).astype(jnp.bfloat16)
    zgate = (summed[:, width : 2 * width] * factor).astype(jnp.bfloat16)
    batch = zpath.shape[0]
    conv = zpath.astype(jnp.float32) * taps[TAPS - 1][None, :]
    for j in range(TAPS - 1):
        conv = conv + buffer[:, j].astype(jnp.float32) * taps[j][None, :]
    new_buffer = jnp.concatenate([buffer[:, 1:], zpath[:, None, :]], axis=1)
    cblocks = conv.reshape(batch, recur_w.shape[0], recur_w.shape[1])
    rgate = jax.nn.sigmoid(
        jnp.einsum("bnc,ncd->bnd", cblocks, recur_w, precision=lax.Precision.HIGHEST).reshape(
            batch, width
        )
    )
    igate = jax.nn.sigmoid(
        jnp.einsum("bnc,ncd->bnd", cblocks, input_matrix, precision=lax.Precision.HIGHEST).reshape(
            batch, width
        )
    )
    loga = 8.0 * rgate * jax.nn.log_sigmoid(logit)[None, :]
    new_hidden = jnp.exp(loga) * hidden + jnp.sqrt(-jnp.expm1(2.0 * loga)) * (igate * conv)
    mixed = (new_hidden * jax.nn.gelu(zgate.astype(jnp.float32))).astype(jnp.bfloat16)
    update = jnp.dot(collect(mixed, "dp", 0), out_w, preferred_element_type=jnp.float32)
    return (update, new_hidden, new_buffer)


def per_device(
    stream_in,
    hidden_state,
    convolution_window_state,
    norm_gain,
    path_weight,
    output_gate_weight,
    conv_taps,
    recur_map,
    input_map,
    decay_logit,
    out_weight,
):
    stream = stream_in
    partial_value = split_inputs(stream, norm_gain[0], path_weight[0], output_gate_weight[0])
    update, hidden_first, buffer_first = recur_tail(
        partial_value,
        hidden_state[0],
        convolution_window_state[0],
        conv_taps[0],
        recur_map[0],
        input_map[0],
        decay_logit[0],
        out_weight[0],
    )
    stream = (
        stream.astype(jnp.float32) + sum_at_owner(update.astype(jnp.bfloat16), "tp", 0)
    ).astype(jnp.bfloat16)
    partial_value = split_inputs(stream, norm_gain[1], path_weight[1], output_gate_weight[1])
    update, hidden_second, buffer_second = recur_tail(
        partial_value,
        hidden_state[1],
        convolution_window_state[1],
        conv_taps[1],
        recur_map[1],
        input_map[1],
        decay_logit[1],
        out_weight[1],
    )
    stream = (
        stream.astype(jnp.float32) + sum_at_owner(update.astype(jnp.bfloat16), "tp", 0)
    ).astype(jnp.bfloat16)
    return (
        stream,
        jnp.stack([hidden_first, hidden_second]),
        jnp.stack([buffer_first, buffer_second]),
    )


def solution(mesh):
    placed = (
        P("tp", "dp"),
        P(None, "dp", "tp"),
        P(None, "dp", None, "tp"),
        P(None, "dp"),
        P(None, "dp", "tp"),
        P(None, "dp", "tp"),
        P(None, None, "tp"),
        P(None, "tp", None, None),
        P(None, "tp", None, None),
        P(None, "tp"),
        P(None, "tp", "dp"),
    )
    return jax.shard_map(
        per_device,
        mesh=mesh,
        in_specs=placed,
        out_specs=(P("tp", "dp"), P(None, "dp", "tp"), P(None, "dp", None, "tp")),
        check_vma=False,
    )
```

```python
import jax
import jax.numpy as jnp
from jax import lax
from jax.experimental import pallas as pl
from jax.experimental.pallas import tpu as pltpu
from jax.sharding import PartitionSpec as P

D = 4096
TAPS = 4
EPS = 1e-06

TP = 16
YS = 4
OWN = 32
ROWS = YS * OWN
COLS = 512
CH = 256
CHUNK = ROWS // TP
MSG = ROWS + OWN + 8


BF = jnp.bfloat16
F32 = jnp.float32


def run(kernel, outs, operands, name, scratch=()):
    vmem = pl.BlockSpec(memory_space=pltpu.VMEM)
    smem = pl.BlockSpec(memory_space=pltpu.SMEM)
    specs = [smem if o.dtype == jnp.int32 else vmem for o in operands]
    single = not isinstance(outs, list)
    return pl.pallas_call(
        kernel,
        out_shape=outs,
        in_specs=specs,
        out_specs=vmem if single else [vmem] * len(outs),
        scratch_shapes=list(scratch),
        compiler_params=pltpu.CompilerParams(vmem_limit_bytes=8 * 1024 * 1024),
        name=name,
    )(*operands)


def shape(*dims, dtype=BF):
    return jax.ShapeDtypeStruct(dims, dtype)


def from_everyone(array, axis):
    return lax.all_to_all(array, axis, split_axis=0, concat_axis=0, tiled=True)


def other_core(array):
    return lax.ppermute(array, "dp", [(i, i ^ 1) for i in range(2 * YS)])


def other_chip(array, k):
    return lax.ppermute(array, "dp", [(i, i ^ (2 * k)) for i in range(2 * YS)])


def spread_kernel(x, out):
    out[...] = jnp.broadcast_to(x[...][None], out.shape)


def give_kernel(where, everyone, out):
    out[...] = everyone[:, 1 - where[1]]


def project(xs, gains, paths, gates, state, msg):
    zp = zg = squares = None
    for x, gain, path, gate in zip(xs, gains, paths, gates, strict=True):
        xf = x.astype(F32)
        gained = (xf * gain).astype(BF)
        p = jnp.dot(gained, path, preferred_element_type=F32)
        g = jnp.dot(gained, gate, preferred_element_type=F32)
        zp = p if zp is None else zp + p
        zg = g if zg is None else zg + g
        for at in range(0, COLS, 128):
            piece = xf[:, at : at + 128]
            squares = piece * piece if squares is None else squares + piece * piece
    msg[:ROWS, :CH] = zp.astype(BF)
    msg[:ROWS, CH:] = zg.astype(BF)
    msg[ROWS : ROWS + OWN, :] = state
    sumsq = jnp.broadcast_to(jnp.sum(jnp.transpose(squares), axis=0, keepdims=True), (8, ROWS))
    high = sumsq.astype(BF)
    low = (sumsq - high.astype(F32)).astype(BF)
    msg[ROWS + OWN :, :ROWS] = high
    msg[ROWS + OWN :, ROWS : 2 * ROWS] = low
    msg[ROWS + OWN :, 2 * ROWS :] = jnp.zeros((8, 2 * CH - 2 * ROWS), BF)


def first_kernel(where, everyone, theirs, gain, gain_o, path, path_o, gate, gate_o, state, msg):
    mine = everyone[:, where[1]].reshape(ROWS, COLS)
    project(
        (mine, theirs[...].reshape(ROWS, COLS)),
        (gain[0:1], gain_o[0:1]),
        (path[0], path_o[0]),
        (gate[0], gate_o[0]),
        state[0],
        msg,
    )


def later_kernel(x, gain, gain_o, path, path_o, gate, gate_o, state, msg):
    xs = x[...].reshape(ROWS, 2 * COLS)
    project(
        (xs[:, :COLS], xs[:, COLS:]),
        (gain[1:2], gain_o[1:2]),
        (path[1], path_o[1]),
        (gate[1], gate_o[1]),
        state[1],
        msg,
    )


def prepare_kernel(hidden, window, taps, recur, inputs, state, blocks):
    blocks[...] = jnp.zeros(blocks.shape, F32)
    for layer in range(2):
        state[layer, :, :CH] = hidden[layer].astype(BF)
        state[layer, :, CH:] = before(window, taps, layer).astype(BF)
        for pair in range(2):
            for half in range(2):
                at = slice(64 * half, 64 * half + 64)
                to = slice(128 + 64 * half, 128 + 64 * half + 64)
                blocks[layer, pair, at, at] = recur[layer, 2 * pair + half]
                blocks[layer, pair, at, to] = inputs[layer, 2 * pair + half]


def before(window, taps, layer):
    total = window[layer, 0].astype(F32) * taps[layer, 0:1]
    for j in range(1, TAPS - 1):
        total = total + window[layer, j].astype(F32) * taps[layer, j : j + 1]
    return total


def tail(layer, where, msgs, hidden, window, taps, blocks, logit, h_all, c_all, z_all, hn, bn):
    y = where[0]
    z = msgs[0][:ROWS].astype(F32)
    stats = msgs[0][ROWS + OWN :, : 2 * ROWS].astype(F32)
    for m in msgs[1:]:
        z = z + m[:ROWS].astype(F32)
        stats = stats + m[ROWS + OWN :, : 2 * ROWS].astype(F32)
    factor = lax.rsqrt((stats[:, :ROWS] + stats[:, ROWS:]) / D + EPS)
    factor = jnp.transpose(jnp.concatenate([factor] * (ROWS // 8), axis=0))
    factor = jnp.concatenate([factor] * 2, axis=1)
    zp = (z[:, :CH] * factor).astype(BF).astype(F32)
    zg = (z[:, CH:] * factor).astype(BF).astype(F32)
    for k in range(1, YS):
        theirs = msgs[k][ROWS : ROWS + OWN].astype(F32)
        rows = pl.ds(pl.multiple_of((y ^ k) * OWN, OWN), OWN)
        h_all[rows] = theirs[:, :CH]
        c_all[rows] = theirs[:, CH:]
    own = pl.ds(pl.multiple_of(y * OWN, OWN), OWN)
    h_all[own] = hidden[layer]
    c_all[own] = before(window, taps, layer)
    conv = c_all[...] + zp * taps[layer, TAPS - 1 : TAPS]
    rates = []
    ins = []
    for pair in range(2):
        both = jnp.dot(
            conv[:, 128 * pair : 128 * pair + 128],
            blocks[layer, pair],
            preferred_element_type=F32,
            precision=lax.Precision.HIGHEST,
        )
        rates.append(both[:, :128])
        ins.append(both[:, 128:])
    rate = jax.nn.sigmoid(jnp.concatenate(rates, axis=1))
    gate = jax.nn.sigmoid(jnp.concatenate(ins, axis=1))
    decay = -8.0 * jnp.log(1.0 + jnp.exp(-logit[layer : layer + 1]))
    loga = rate * decay
    a = jnp.exp(loga)
    twice = 2.0 * loga
    series = -twice * (1.0 + twice * (0.5 + twice * (1.0 / 6.0 + twice * (1.0 / 24.0))))
    rest = jnp.where(twice > -0.05, series, 1.0 - a * a)
    h = a * h_all[...] + jnp.sqrt(rest) * (gate * conv)
    h_all[...] = h
    z_all[...] = zp
    hn[...] = h_all[own]
    bn[0] = window[layer, 1]
    bn[1] = window[layer, 2]
    bn[2] = z_all[own].astype(BF)
    return (h * jax.nn.gelu(zg)).astype(BF)


def first_tail_kernel(
    where, m0, m1, m2, m3, hidden, window, taps, blocks, logit, out_w, out_w_o, upd, hn, bn,
    h_all, c_all, z_all,
):
    mixed = tail(
        0, where, (m0, m1, m2, m3), hidden, window, taps, blocks, logit, h_all, c_all, z_all, hn, bn
    )
    own = jnp.dot(mixed, out_w[0], preferred_element_type=F32)
    upd[:, :, :COLS] = own.astype(BF).reshape(TP, CHUNK, COLS)
    other = jnp.dot(mixed, out_w_o[0], preferred_element_type=F32)
    upd[:, :, COLS:] = other.astype(BF).reshape(TP, CHUNK, COLS)


def later_tail_kernel(
    where, m0, m1, m2, m3, hidden, window, taps, blocks, logit, out_w, out_w_o, x, hn0, bn0,
    keep, give, hn, bn, h_all, c_all, z_all, upd,
):
    mixed = tail(
        1, where, (m0, m1, m2, m3), hidden, window, taps, blocks, logit, h_all, c_all, z_all,
        hn.at[1], bn.at[1],
    )
    hn[0] = hn0[...]
    bn[0] = bn0[...]
    t = where[2]
    other = jnp.dot(mixed, out_w_o[1], preferred_element_type=F32)
    upd[...] = other.reshape(TP, CHUNK, COLS)
    upd[t] += x[t, :, COLS:].astype(F32)
    give[...] = upd[...].astype(BF).reshape(YS, OWN, COLS)
    own = jnp.dot(mixed, out_w[1], preferred_element_type=F32)
    upd[...] = own.reshape(TP, CHUNK, COLS)
    upd[t] += x[t, :, :COLS].astype(F32)
    keep[...] = upd[...].astype(BF).reshape(YS, OWN, COLS)


def middle_kernel(where, parts, everyone, theirs, out):
    t = where[2]
    total = jnp.sum(parts[...].astype(F32), axis=0)
    at = pl.ds(pl.multiple_of((t % 4) * CHUNK, CHUNK), CHUNK)
    own = everyone[t // 4, where[1], at, :].astype(F32)
    other = theirs[t // 4, at, :].astype(F32)
    x = (jnp.concatenate([own, other], axis=1) + total).astype(BF)
    out[...] = jnp.broadcast_to(x[None], out.shape)


def join_kernel(where, keep, theirs, out):
    c = where[1]
    out[:, c] = keep[...]
    out[:, 1 - c] = theirs[...]


def last_kernel(parts, out):
    out[...] = jnp.sum(parts[...].astype(F32), axis=0).astype(BF)


def exchange(msg):
    return (msg, *(other_chip(msg, k) for k in range(1, YS)))


def per_device(
    stream_in,
    hidden_state,
    convolution_window_state,
    norm_gain,
    path_weight,
    output_gate_weight,
    conv_taps,
    recur_map,
    input_map,
    decay_logit,
    out_weight,
):
    dp = lax.axis_index("dp")
    where = jnp.stack([dp // 2, dp % 2, lax.axis_index("tp")]).astype(jnp.int32)
    window = jnp.transpose(convolution_window_state, (0, 2, 1, 3))
    gain_o, path_o, gate_o, out_o = (
        other_core(w) for w in (norm_gain, path_weight, output_gate_weight, out_weight)
    )
    spread = run(spread_kernel, shape(TP, 16, COLS), (stream_in,), "spread")
    everyone = from_everyone(spread, "tp").reshape(YS, 2, OWN, COLS)
    state, blocks = run(
        prepare_kernel,
        [shape(2, OWN, 2 * CH), shape(2, 2, 128, 256, dtype=F32)],
        (hidden_state, window, conv_taps, recur_map, input_map),
        "prepare",
    )
    theirs = other_core(run(give_kernel, shape(YS, OWN, COLS), (where, everyone), "give"))
    msg = run(
        first_kernel,
        shape(MSG, 2 * CH),
        (where, everyone, theirs, norm_gain, gain_o, path_weight, path_o, output_gate_weight, gate_o, state),
        "first",
    )
    scratch = [pltpu.VMEM((ROWS, CH), F32)] * 3
    common = (hidden_state, window, conv_taps, blocks, decay_logit, out_weight, out_o)
    upd, hn0, bn0 = run(
        first_tail_kernel,
        [shape(TP, CHUNK, 2 * COLS), shape(OWN, CH, dtype=F32), shape(TAPS - 1, OWN, CH)],
        (where, *exchange(msg), *common),
        "first_tail",
        scratch,
    )
    parts = from_everyone(upd, "tp")
    x = run(middle_kernel, shape(TP, CHUNK, 2 * COLS), (where, parts, everyone, theirs), "middle")
    x = from_everyone(x, "tp")
    msg = run(
        later_kernel,
        shape(MSG, 2 * CH),
        (x, norm_gain, gain_o, path_weight, path_o, output_gate_weight, gate_o, state),
        "later",
    )
    keep, give, hn, bn = run(
        later_tail_kernel,
        [
            shape(YS, OWN, COLS),
            shape(YS, OWN, COLS),
            shape(2, OWN, CH, dtype=F32),
            shape(2, TAPS - 1, OWN, CH),
        ],
        (where, *exchange(msg), *common, x, hn0, bn0),
        "later_tail",
        [*scratch, pltpu.VMEM((TP, CHUNK, COLS), F32)],
    )
    joined = run(
        join_kernel, shape(YS, 2, OWN, COLS), (where, keep, other_core(give)), "join"
    )
    parts = from_everyone(joined.reshape(TP, 16, COLS), "tp")
    stream = run(last_kernel, shape(16, COLS), (parts,), "last")
    return stream, hn, jnp.transpose(bn, (0, 2, 1, 3))


def solution(mesh):
    placed = (
        P("tp", "dp"),
        P(None, "dp", "tp"),
        P(None, "dp", None, "tp"),
        P(None, "dp"),
        P(None, "dp", "tp"),
        P(None, "dp", "tp"),
        P(None, None, "tp"),
        P(None, "tp", None, None),
        P(None, "tp", None, None),
        P(None, "tp"),
        P(None, "tp", "dp"),
    )
    return jax.shard_map(
        per_device,
        mesh=mesh,
        in_specs=placed,
        out_specs=(P("tp", "dp"), P(None, "dp", "tp"), P(None, "dp", None, "tp")),
        check_vma=False,
    )
```
